32 devices in a mesh: ep: 16 (over z, y, x), tp: 2 (over core).
Axes of the slice: x: 2, y: 2, z: 4, core: 2. Of those that a mesh axis runs over, the one named last changes fastest.
Arguments:
- tokens: bfloat16 [2048, 2048], P('ep', 'tp'), may hold values from -6 to 6
- cotangent: bfloat16 [2048, 2048], P('ep', 'tp'), may hold values from -6 to 6
- routes: int32 [2048, 2], P('ep'), may hold values from 0 to 15, all different within a row; in each aligned block of 128 rows (0 to 127, 128 to 255, ...) at most 24 rows name the same one
- route_weights: float32 [2048, 2], P('ep'), may hold values from 0.1 to 2.5
- gate_proj: bfloat16 [16, 2048, 512], P('ep', None, 'tp'), may hold values from -0.125 to 0.125
- up_proj: bfloat16 [16, 2048, 512], P('ep', None, 'tp'), may hold values from -0.125 to 0.125
- down_proj: bfloat16 [16, 512, 2048], P('ep', 'tp'), may hold values from -0.25 to 0.25
- shared_gate: bfloat16 [2048, 512], P(None, 'tp'), may hold values from -0.125 to 0.125
- shared_up: bfloat16 [2048, 512], P(None, 'tp'), may hold values from -0.125 to 0.125
- shared_down: bfloat16 [2048, 512], P(None, 'tp'), may hold values from -0.25 to 0.25
Outputs:
- token_grad: bfloat16 [2048, 2048], P('ep', 'tp')
- weight_grad: float32 [2048, 2], P('ep')
- gate_grad: bfloat16 [16, 2048, 512], P('ep', None, 'tp')
- up_grad: bfloat16 [16, 2048, 512], P('ep', None, 'tp')
- down_grad: bfloat16 [16, 512, 2048], P('ep', 'tp')
- sharedgate_grad: float32 [2048, 512], P('ep', 'tp')
- sharedup_grad: float32 [2048, 512], P('ep', 'tp')
- shareddown_grad: float32 [2048, 512], P('ep', 'tp')
The draws below stay inside these ranges and needn't reach their ends.
Inputs may be any that keep to these rules, and one draw needn't show every extreme that they name: `routes`: the 2 entries of a token name different experts. Among the 128 tokens of one group no expert is named more than 24 times, and in some groups an expert is named exactly 24 times.
All inputs are finite; a program needn't handle non-finite values.
Results may differ from the reference program's by a relative error of at most 0.007.
Values may be sent and summed in bfloat16 or wider, within the bound.
No kernel may reach another device: no remote copies, remote signals or barrier semaphores. Data moves between devices by JAX's collectives and lax.ppermute only.
A program may use at most 128 MiB of HBM per device.

```python
import math
import jax
import jax.numpy as jnp
import numpy as np
from jax import lax

D = 2048
F = 512
FS = 512
TOP_K = 2
TOK_DEV = 128
EXPERTS = 16
TOKENS = 2048
CAP = 24
N_EP = 16
N_TP = 2


def strengthened(result, key, source, target, shards_of, factor):
    def block_of(position):
        return (jnp.arange(result.shape[position]) // (result.shape[position] // shards_of)).reshape((-1,) + (1,) * (result.ndim - 1 - position))

    one_side = jax.random.permutation(key, shards_of)[block_of(target)]
    other_side = (block_of(target) + shards_of // 2) % shards_of
    return jnp.where((block_of(source) == one_side) | (block_of(source) == other_side), factor * result, result)


def block_levels(rng, dims, pieces, smallest, high):
    def one(dim, blocks):
        steps = jax.random.uniform(jax.random.fold_in(jax.random.fold_in(rng, 6), dim), (blocks,), jnp.float32, smallest / len(pieces), high / len(pieces))
        return jnp.repeat(jnp.exp(steps), dims[dim] // blocks).reshape((-1,) + (1,) * (len(dims) - dim - 1))

    factor_of = one(*pieces[0])
    for cut in pieces[1:]:
        factor_of = factor_of * one(*cut)
    return factor_of


def deal_out(stream_key, own, number, rows, number_of, top, most, slope):
    sequence = jax.random.permutation(stream_key, number_of)
    crowded, common = portions_of(number_of, rows * top, most, slope, True), portions_of(number_of, rows * top, most, slope, False)
    places = jnp.arange(number_of)

    def named(lengths, offset_by):
        used = int((lengths > 0).sum())
        fixed = max(1, used // 4)
        moved = fixed + (places - fixed + offset_by * (used - fixed)) % max(1, number_of - fixed)
        return jnp.zeros((number_of,), jnp.int32).at[sequence[jnp.where(places < fixed, places, moved)]].set(jnp.asarray(lengths, jnp.int32))

    lengths = jnp.where(number % 4 == 0, named(crowded, number // 4), named(common, number - number // 4 - 1))
    mixed = jax.random.permutation(jax.random.fold_in(own, 3), number_of)
    source_of, taker = mixed[0:number_of // 2 * 2:2], mixed[1:number_of // 2 * 2:2]
    slack = jnp.minimum(lengths[source_of] - 1, most - lengths[taker]) // 2
    slack = jnp.where((source_of == sequence[0]) | (taker == sequence[0]) | (lengths[taker] == 0), 0, jnp.maximum(slack, 0))
    moved = jax.random.randint(jax.random.fold_in(own, 4), (number_of // 2,), 0, 1 << 20) % (slack + 1)
    lengths = lengths.at[source_of].add(-moved).at[taker].add(moved)
    members = jnp.searchsorted(jnp.cumsum(lengths), jnp.arange(rows * top), side="right").astype(jnp.int32)
    grid = members.reshape(top, rows).T
    grid = grid[jax.random.permutation(jax.random.fold_in(own, 1), rows)]
    offset_by = jax.random.randint(jax.random.fold_in(own, 2), (rows, 1), 0, top)
    return jnp.take_along_axis(grid, (jnp.arange(top)[None, :] + offset_by) % top, axis=1)


def portions_of(number_of, total, limit, skew, full):
    portions = [(1 << 20) // math.isqrt(rank ** skew) + 1 for rank in range(1, number_of + 1)]
    largest = limit if full else min(limit, max(-(-total // number_of), total * portions[0] // sum(portions)))
    least = 1 if total - largest >= number_of - 1 else 0
    given, rest = [largest] + [least] * (number_of - 1), total - largest - least * (number_of - 1)
    while rest > 0:
        movable = [i for i in range(1, number_of) if given[i] < largest] or [i for i in range(1, number_of) if given[i] < limit]
        whole, budget = sum([portions[i] for i in movable]), rest
        for i in movable:
            extra = min(limit - given[i], max(1, budget * portions[i] // whole), rest)
            given[i] = given[i] + extra
            rest = rest - extra
    return np.array(given)


def centred(key, shape, deviation, most, shards=(), kind=jnp.bfloat16):
    entries = jax.random.normal(key, shape, jnp.float32) * deviation
    if len(shards) > 0:
        entries = block_levels(key, shape, shards, -0.22, 0.18) * entries
    return jnp.clip(entries, min=-most, max=most).astype(kind)


def gaussian_with(stream_key, extent, spread, limit, shards, heavy, held_as=jnp.bfloat16):
    entries = spread * jax.random.normal(stream_key, extent, jnp.float32)
    if shards:
        entries = entries * block_levels(stream_key, extent, shards, -0.22, 0.18)
    return jnp.clip(strengthened(entries, jax.random.fold_in(stream_key, 3), *heavy), -limit, limit).astype(held_as)


def setup_inputs(seed: int = 0) -> dict:
    streams_of = jax.random.split(jax.random.key(seed), 11)
    tokens = gaussian_with(streams_of[0], (TOKENS, D), 1.0, 6.0, ((0, 16), (1, 2)), (0, 1, 16, 2.0))
    cotangent = gaussian_with(streams_of[1], (TOKENS, D), 1.0, 6.0, ((0, 16), (1, 2)), (0, 1, 16, 2.0))
    routes_keys = jax.random.split(jax.random.fold_in(streams_of[2], 1), TOKENS // TOK_DEV)
    routes_turns = jax.random.permutation(jax.random.fold_in(streams_of[2], 3), TOKENS // TOK_DEV)
    routes = jax.vmap(lambda own, number: deal_out(jax.random.fold_in(streams_of[2], 2), own, number, TOK_DEV, EXPERTS, TOP_K, CAP, 1))(routes_keys, routes_turns).reshape((TOKENS, TOP_K))
    route_weights = jnp.clip(jnp.exp(math.log(2.5) - 3.218876 * jax.random.uniform(streams_of[3], (TOKENS, TOP_K), jnp.float32) ** block_levels(streams_of[3], (TOKENS, TOP_K), ((0, 16),), -0.2, 0.2)), 0.1, 2.5)
    gate_proj = centred(streams_of[4], (EXPERTS, D, F), D ** -0.5, 0.125, ((0, 16), (2, 2)))
    up_proj = centred(streams_of[5], (EXPERTS, D, F), D ** -0.5, 0.125, ((0, 16), (2, 2)))
    down_proj = centred(streams_of[6], (EXPERTS, F, D), F ** -0.5, 0.25, ((0, 16), (1, 2)))
    shared_gate = centred(streams_of[7], (D, FS), D ** -0.5, 0.125, ((1, 2),))
    shared_up = centred(streams_of[8], (D, FS), D ** -0.5, 0.125, ((1, 2),))
    shared_down = centred(streams_of[9], (D, FS), FS ** -0.5, 0.25, ((1, 2),))
    return dict(tokens=tokens, cotangent=cotangent, routes=routes, route_weights=route_weights, gate_proj=gate_proj, up_proj=up_proj, down_proj=down_proj, shared_gate=shared_gate, shared_up=shared_up, shared_down=shared_down)


def slot_table(routes, experts, capacity):
    assigned = routes.shape[0] * routes.shape[1]
    flat_routes = routes.reshape(assigned).astype(jnp.int32)
    onehot = (flat_routes[:, None] == jnp.arange(experts, dtype=jnp.int32)[None, :]).astype(jnp.int32)
    before = jnp.cumsum(onehot, axis=0) - onehot
    slot_rank = jnp.sum(before * onehot, axis=1).astype(jnp.int32)
    slot_of = (flat_routes * capacity + slot_rank).astype(jnp.int32)
    empty = jnp.full((experts * capacity,), assigned, jnp.int32)
    slot_owner = empty.at[slot_of].set(jnp.arange(assigned, dtype=jnp.int32))
    return slot_of, slot_owner


def silu_parts(preact):
    sigmoid_v = jax.nn.sigmoid(preact)
    return preact * sigmoid_v, sigmoid_v * (1.0 + preact * (1.0 - sigmoid_v))


def rounded(partial_value):
    return lax.optimization_barrier(partial_value.astype(jnp.bfloat16)).astype(jnp.float32)


def contract_rows(left, right):
    return lax.dot_general(left, right, (((0,), (0,)), ((), ())), preferred_element_type=jnp.float32)


def contract_cols(left, right):
    return lax.dot_general(left, right, (((1,), (1,)), ((), ())), preferred_element_type=jnp.float32)


def reference(tokens, cotangent, routes, route_weights, gate_proj, up_proj, down_proj, shared_gate, shared_up, shared_down):
    assigned = TOK_DEV * TOP_K
    row_width = tokens.shape[1]
    block_size = F // N_TP
    slot_of, slot_owner = jax.vmap(lambda device_routes: slot_table(device_routes, EXPERTS, CAP))(
        routes.reshape(N_EP, TOK_DEV, TOP_K))
    filled = slot_owner < assigned
    owner_safe = jnp.minimum(slot_owner, assigned - 1)
    source = jnp.arange(N_EP, dtype=jnp.int32)[:, None]
    token_at = (source * TOK_DEV + owner_safe // TOP_K).astype(jnp.int32)
    assign_at = (source * assigned + owner_safe).astype(jnp.int32)
    flat_weights = route_weights.reshape(N_EP * assigned)
    weight_at = jnp.where(filled, flat_weights[assign_at], jnp.zeros((), jnp.float32))

    def by_expert(layout):
        return jnp.swapaxes(layout.reshape(N_EP, EXPERTS, CAP), 0, 1).reshape(EXPERTS, N_EP * CAP)

    def expert_step(running, inputs):
        input_acc, weight_acc = running
        token_index, assign_index, slot_weights, slot_live, gate_mat, up_mat, down_mat = inputs
        slot_rows = jnp.where(slot_live[:, None], tokens[token_index], jnp.zeros((), jnp.bfloat16))
        slot_cot = (slot_weights[:, None] * cotangent[token_index].astype(jnp.float32)).astype(jnp.bfloat16)
        gate_pre = jnp.dot(slot_rows, gate_mat, preferred_element_type=jnp.float32)
        up_pre = jnp.dot(slot_rows, up_mat, preferred_element_type=jnp.float32)
        gate_act, gate_slope = silu_parts(gate_pre)
        hidden = gate_act * up_pre
        back_grad = contract_cols(slot_cot, down_mat)
        hidden_low = hidden.astype(jnp.bfloat16)
        down_grad = contract_rows(hidden_low, slot_cot).astype(jnp.bfloat16)
        gate_delta = (back_grad * up_pre * gate_slope).astype(jnp.bfloat16)
        up_delta = (back_grad * gate_act).astype(jnp.bfloat16)
        gate_grad = contract_rows(slot_rows, gate_delta).astype(jnp.bfloat16)
        up_grad = contract_rows(slot_rows, up_delta).astype(jnp.bfloat16)
        slot_sum = jnp.zeros((slot_rows.shape[0], row_width), jnp.float32)
        product_sum = jnp.zeros((slot_rows.shape[0],), jnp.float32)
        for block_index in range(N_TP):
            start_col = block_index * block_size
            stop_col = start_col + block_size
            partial_value = contract_cols(gate_delta[:, start_col:stop_col], gate_mat[:, start_col:stop_col])
            partial_value = partial_value + contract_cols(up_delta[:, start_col:stop_col], up_mat[:, start_col:stop_col])
            slot_sum = slot_sum + rounded(partial_value)
            product_sum = product_sum + rounded(jnp.sum(hidden[:, start_col:stop_col] * back_grad[:, start_col:stop_col], axis=1))
        slot_low = rounded(slot_sum)
        product_low = rounded(product_sum)
        input_acc = input_acc.at[token_index].add(jnp.where(slot_live[:, None], slot_low, jnp.zeros((), jnp.float32)))
        weight_acc = weight_acc.at[assign_index].add(jnp.where(slot_live, product_low, jnp.zeros((), jnp.float32)))
        return (input_acc, weight_acc), (gate_grad, up_grad, down_grad)

    start_acc = (jnp.zeros((TOKENS, row_width), jnp.float32), jnp.zeros((TOKENS * TOP_K,), jnp.float32))
    (input_acc, weight_acc), (gate_grad, up_grad, down_grad) = lax.scan(
        expert_step, start_acc,
        (by_expert(token_at), by_expert(assign_at), by_expert(weight_at), by_expert(filled), gate_proj, up_proj, down_proj))

    mix_gate = jnp.dot(tokens, shared_gate, preferred_element_type=jnp.float32)
    mix_up = jnp.dot(tokens, shared_up, preferred_element_type=jnp.float32)
    mix_act, mix_slope = silu_parts(mix_gate)
    mix_hidden = (mix_act * mix_up).astype(jnp.bfloat16)
    mix_back = jnp.dot(cotangent, shared_down, preferred_element_type=jnp.float32)
    mixgrad_gate = (mix_back * mix_up * mix_slope).astype(jnp.bfloat16)
    mixgrad_up = (mix_back * mix_act).astype(jnp.bfloat16)
    mix_block = FS // N_TP
    mix_input = jnp.zeros((TOKENS, row_width), jnp.float32)
    for block_index in range(N_TP):
        start_col = block_index * mix_block
        stop_col = start_col + mix_block
        partial_value = contract_cols(mixgrad_gate[:, start_col:stop_col], shared_gate[:, start_col:stop_col])
        partial_value = partial_value + contract_cols(mixgrad_up[:, start_col:stop_col], shared_up[:, start_col:stop_col])
        mix_input = mix_input + rounded(partial_value)
    token_grad = (mix_input + input_acc).astype(jnp.bfloat16)
    weight_grad = weight_acc.reshape(TOKENS, TOP_K) / route_weights
    sharedgate_grad = contract_rows(tokens, mixgrad_gate)
    sharedup_grad = contract_rows(tokens, mixgrad_up)
    shareddown_grad = contract_rows(cotangent, mix_hidden)
    return (token_grad, weight_grad, gate_grad, up_grad, down_grad, sharedgate_grad, sharedup_grad, shareddown_grad)
```

```python
import functools

import jax
import jax.numpy as jnp
from jax import lax
from jax.experimental import pallas as pl
from jax.experimental.pallas import tpu as pltpu
from jax.sharding import PartitionSpec as P


BF16 = jnp.bfloat16
F32 = jnp.float32
LANES = 128
VMEM = pl.BlockSpec(memory_space=pltpu.VMEM)
SMEM = pl.BlockSpec(memory_space=pltpu.SMEM)


def dot(left, right, dims=((1,), (0,))):
    return lax.dot_general(left, right, (dims, ((), ())), preferred_element_type=F32)


def silu_parts(preact):
    sigmoid_v = jax.nn.sigmoid(preact)
    return (preact * sigmoid_v, sigmoid_v * (1.0 + preact * (1.0 - sigmoid_v)))


def params(mib):
    return pltpu.CompilerParams(vmem_limit_bytes=mib * 1024 * 1024)


def cost(flops, moved):
    return pl.CostEstimate(flops=flops, bytes_accessed=moved, transcendentals=0)


def pack_kernel(experts, capacity, lane_routes, lane_weights, routes, tokens, cotangent, packed, slots):
    rows, cols = tokens.shape
    total = experts * capacity
    token_a = lax.broadcasted_iota(jnp.int32, (rows, rows), 0)
    token_b = lax.broadcasted_iota(jnp.int32, (rows, rows), 1)
    name_a = lax.broadcasted_iota(jnp.int32, (experts, rows), 0)
    hot0 = (lane_routes[0:1, :] == name_a).astype(F32)
    hot1 = (lane_routes[1:2, :] == name_a).astype(F32)
    before = dot((hot0 + hot1).astype(BF16), (token_a < token_b).astype(F32).astype(BF16))
    slot0 = lane_routes[0:1, :] * capacity + jnp.sum(hot0 * before, axis=0, keepdims=True).astype(jnp.int32)
    slot1 = lane_routes[1:2, :] * capacity + jnp.sum(hot1 * before, axis=0, keepdims=True).astype(jnp.int32)
    place = lax.broadcasted_iota(jnp.int32, (total, rows), 0)
    pick0 = (place == slot0).astype(F32)
    pick1 = (place == slot1).astype(F32)
    weight = jnp.sum(pick0 * lane_weights[0:1, :] + pick1 * lane_weights[1:2, :], axis=1, keepdims=True)
    pick = (pick0 + pick1).astype(BF16)
    packed[:, :cols] = dot(pick, tokens[...]).astype(BF16)
    packed[:, cols:] = (dot(pick, cotangent[...]) * weight).astype(BF16)
    name_b = lax.broadcasted_iota(jnp.int32, (rows, experts), 1)
    col0 = (routes[:, 0:1] == name_b).astype(F32)
    col1 = (routes[:, 1:2] == name_b).astype(F32)
    ahead = dot((token_b < token_a).astype(F32).astype(BF16), (col0 + col1).astype(BF16))
    slots[:, 0:1] = routes[:, 0:1] * capacity + jnp.sum(col0 * ahead, axis=1, keepdims=True).astype(jnp.int32)
    slots[:, 1:2] = routes[:, 1:2] * capacity + jnp.sum(col1 * ahead, axis=1, keepdims=True).astype(jnp.int32)


def mix_kernel(core, own_x, other_x, own_c, other_c, gate, up, down, grads, keep, send):
    cols = own_x.shape[1]
    hidden = gate.shape[1]
    mine = pl.ds(pl.multiple_of(core[0] * cols, cols), cols)
    theirs = pl.ds(pl.multiple_of((1 - core[0]) * cols, cols), cols)
    pre = dot(own_x[...], gate[mine, :]) + dot(other_x[...], gate[theirs, :])
    mix_up = dot(own_x[...], up[mine, :]) + dot(other_x[...], up[theirs, :])
    back = dot(own_c[...], down[mine, :]) + dot(other_c[...], down[theirs, :])
    act, slope = silu_parts(pre)
    gate_delta = (back * mix_up * slope).astype(BF16)
    up_delta = (back * act).astype(BF16)
    grads[:, :hidden] = gate_delta
    grads[:, hidden : 2 * hidden] = up_delta
    grads[:, 2 * hidden :] = (act * mix_up).astype(BF16)
    lanes = ((1,), (1,))
    send[...] = (dot(gate_delta, gate[theirs, :], lanes) + dot(up_delta, up[theirs, :], lanes)).astype(BF16)
    keep[...] = (dot(gate_delta, gate[mine, :], lanes) + dot(up_delta, up[mine, :], lanes)).astype(BF16)


def outer_kernel(place, own_x, other_x, own_c, other_c, grads, *rest):
    outs, (full_x, full_c) = rest[:-2], rest[-2:]
    cols = own_x.shape[1]
    block = outs[0].shape[1]
    hidden = grads.shape[1] // 3
    half = grads.shape[1] // 2
    core, me = place[0], place[1]
    mine = pl.ds(pl.multiple_of(core * cols, cols), cols)
    theirs = pl.ds(pl.multiple_of((1 - core) * cols, cols), cols)
    full_x[:, mine] = own_x[...]
    full_x[:, theirs] = other_x[...]
    full_c[:, mine] = own_c[...]
    full_c[:, theirs] = other_c[...]
    count = 2 * cols // block
    spots = [[0, 0], [0, 0]]
    for k in range(count):
        at = pl.ds(pl.multiple_of(jnp.bitwise_xor(me, k) * block, block), block)
        rows_ = ((0,), (0,))
        from_x = dot(full_x[:, at], grads[:, : 2 * hidden], rows_).astype(BF16)
        from_c = dot(full_c[:, at], grads[:, 2 * hidden :], rows_).astype(BF16)
        for side in range(2):
            sent = (k >> side) & 1
            out, spot = outs[2 * side + sent], spots[side][sent]
            spots[side][sent] += 1
            if side == 0:
                out[spot] = from_x[:, :half]
            else:
                out[spot, :, : 2 * hidden - half] = from_x[:, half:]
                out[spot, :, 2 * hidden - half :] = from_c


def expert_kernel(core, own, other, gate, up, down, hidden_low, gate_out, up_out, keep, send):
    cols = own.shape[1] // 2
    mine = pl.ds(pl.multiple_of(core[0] * cols, cols), cols)
    theirs = pl.ds(pl.multiple_of((1 - core[0]) * cols, cols), cols)
    lanes = ((1,), (1,))
    pre = dot(own[:, :cols], gate[mine, :]) + dot(other[:, :cols], gate[theirs, :])
    up_pre = dot(own[:, :cols], up[mine, :]) + dot(other[:, :cols], up[theirs, :])
    back = dot(own[:, cols:], down[:, mine], lanes) + dot(other[:, cols:], down[:, theirs], lanes)
    act, slope = silu_parts(pre)
    hidden = act * up_pre
    hidden_low[...] = hidden.astype(BF16)
    product = jnp.sum(hidden * back, axis=1, keepdims=True)
    gate_delta = (back * up_pre * slope).astype(BF16)
    up_delta = (back * act).astype(BF16)
    gate_out[...] = gate_delta
    up_out[...] = up_delta
    spread = jnp.broadcast_to(product, (product.shape[0], LANES)).astype(BF16)
    send[:, :cols] = (dot(gate_delta, gate[theirs, :], lanes) + dot(up_delta, up[theirs, :], lanes)).astype(BF16)
    send[:, cols:] = spread
    keep[:, :cols] = (dot(gate_delta, gate[mine, :], lanes) + dot(up_delta, up[mine, :], lanes)).astype(BF16)
    keep[:, cols:] = spread


def home_kernel(slots, weights, home, mix_a, mix_b, token_grad, weight_grad):
    rows, cols = token_grad.shape
    place = lax.broadcasted_iota(jnp.int32, (rows, home.shape[0]), 1)
    pick0 = (place == slots[:, 0:1]).astype(F32)
    pick1 = (place == slots[:, 1:2]).astype(F32)
    routed = dot((pick0 + pick1).astype(BF16), home[:, :cols])
    token_grad[...] = (mix_a[...].astype(F32) + mix_b[...].astype(F32) + routed).astype(BF16)
    tail = home[:, cols:]
    weight_grad[:, 0:1] = dot(pick0.astype(BF16), tail)[:, 0:1] / weights[:, 0:1]
    weight_grad[:, 1:2] = dot(pick1.astype(BF16), tail)[:, 0:1] / weights[:, 1:2]


def shape(dims, dtype=BF16):
    return jax.ShapeDtypeStruct(dims, dtype)


def per_device(
    tokens,
    cotangent,
    routes,
    route_weights,
    gate_proj,
    up_proj,
    down_proj,
    shared_gate,
    shared_up,
    shared_down,
):
    groups = lax.axis_size("ep")
    halves = lax.axis_size("tp")
    assert halves == 2 and gate_proj.shape[0] == 1
    me, core = lax.axis_index("ep"), lax.axis_index("tp")
    experts = groups
    rows, top = routes.shape
    assert top == 2
    cols = tokens.shape[1]
    hidden = gate_proj.shape[2]
    mix_hidden = shared_gate.shape[1]
    assigned = rows * top
    capacity = assigned // experts + assigned // (2 * experts)
    total = experts * capacity
    core_arr = core.astype(jnp.int32).reshape(1)
    place_arr = jnp.stack([core, me]).astype(jnp.int32)

    def swap(value):
        return lax.ppermute(value, "tp", [(0, 1), (1, 0)])

    def cross(value, bit):
        return lax.ppermute(value, "ep", [(i, i ^ (1 << bit)) for i in range(groups)])

    other_x, other_c = swap(tokens), swap(cotangent)
    packed, slots = pl.pallas_call(
        functools.partial(pack_kernel, experts, capacity),
        out_shape=(shape((total, 2 * cols)), shape((rows, top), jnp.int32)),
        in_specs=[VMEM] * 5,
        out_specs=(VMEM, VMEM),
        cost_estimate=cost(4 * total * rows * cols, 6 * total * cols),
        name="pack",
    )(routes.T, route_weights.T, routes, tokens, cotangent)
    got = lax.all_to_all(
        packed.reshape(groups, capacity, 2 * cols), "ep", split_axis=0, concat_axis=0, tiled=True
    ).reshape(total, 2 * cols)

    grads, mix_keep, mix_send = pl.pallas_call(
        mix_kernel,
        out_shape=(shape((rows, 3 * mix_hidden)), shape((rows, cols)), shape((rows, cols))),
        in_specs=[SMEM] + [VMEM] * 7,
        out_specs=(VMEM,) * 3,
        cost_estimate=cost(20 * rows * cols * mix_hidden, 12 * cols * mix_hidden),
        name="mix",
    )(core_arr, tokens, other_x, cotangent, other_c, shared_gate, shared_up, shared_down)
    mix_got = swap(mix_send)
    block = 2 * cols // groups
    width = 3 * mix_hidden // 2
    bits = groups.bit_length() - 1
    assert groups == 1 << bits and bits >= 2
    orders = [list(range(bits)), [1, 0] + list(range(2, bits))]
    if block % LANES == 0 and width % LANES == 0:
        part = shape((groups // 2, block, width))
        keep_a, send_a, keep_b, send_b = pl.pallas_call(
            outer_kernel,
            out_shape=(part,) * 4,
            in_specs=[SMEM] + [VMEM] * 5,
            out_specs=(VMEM,) * 4,
            scratch_shapes=[pltpu.VMEM((rows, 2 * cols), BF16)] * 2,
            cost_estimate=cost(12 * rows * cols * mix_hidden, 12 * cols * mix_hidden),
            name="outer",
        )(place_arr, tokens, other_x, cotangent, other_c, grads)
    else:
        first = core == 0
        full_x = jnp.where(first, jnp.concatenate([tokens, other_x], 1), jnp.concatenate([other_x, tokens], 1))
        full_c = jnp.where(first, jnp.concatenate([cotangent, other_c], 1), jnp.concatenate([other_c, cotangent], 1))
        stacked = jnp.concatenate(
            [dot(full_x, grads[:, : 2 * mix_hidden], ((0,), (0,))), dot(full_c, grads[:, 2 * mix_hidden :], ((0,), (0,)))],
            axis=1,
        ).astype(BF16)
        blocks = jnp.take(stacked.reshape(groups, block, -1), me ^ jnp.arange(groups), axis=0)
        numbers = list(range(groups))

        def those(side, value):
            return blocks[jnp.array([k for k in numbers if (k >> side) & 1 == value])][:, :, side * width : (side + 1) * width]

        keep_a, send_a, keep_b, send_b = those(0, 0), those(0, 1), those(1, 0), those(1, 1)
    sums = []
    for keep, send, order in ((keep_a, send_a, orders[0]), (keep_b, send_b, orders[1])):
        left = [k for k in range(groups) if not (k >> order[0]) & 1]
        value = keep.astype(F32) + cross(send, order[0]).astype(F32)
        go = [i for i, k in enumerate(left) if (k >> order[1]) & 1]
        stay = [i for i, k in enumerate(left) if not (k >> order[1]) & 1]
        pairs = value.reshape((-1, 2) + value.shape[1:])
        assert stay == list(range(0, len(left), 2)) and go == list(range(1, len(left), 2))
        sums.append(pairs[:, 0] + cross(pairs[:, 1].astype(BF16), order[1]).astype(F32))
    value = jnp.concatenate(sums, axis=2)
    for bit in range(2, bits):
        pairs = value.reshape((-1, 2) + value.shape[1:])
        value = pairs[:, 0] + cross(pairs[:, 1].astype(BF16), bit).astype(F32)
    stacked = value[0]

    got_other = swap(got)
    hidden_low, gate_delta, up_delta, keep, send = pl.pallas_call(
        expert_kernel,
        out_shape=(shape((total, hidden)),) * 3 + (shape((total, cols + LANES)),) * 2,
        in_specs=[SMEM] + [VMEM] * 5,
        out_specs=(VMEM,) * 5,
        cost_estimate=cost(20 * total * cols * hidden, 12 * cols * hidden),
        name="expert",
    )(core_arr, got, got_other, gate_proj[0], up_proj[0], down_proj[0])
    back = (keep.astype(F32) + swap(send).astype(F32)).astype(BF16)
    home = lax.all_to_all(
        back.reshape(groups, capacity, cols + LANES), "ep", split_axis=0, concat_axis=0, tiled=True
    ).reshape(total, cols + LANES)

    def ordered(own, other):
        return jnp.concatenate([jnp.where(core == 0, own, other), jnp.where(core == 0, other, own)], axis=1)

    slot_rows = ordered(got[:, :cols], got_other[:, :cols])
    slot_cot = ordered(got[:, cols:], got_other[:, cols:])
    over = ((0,), (0,))
    gate_grad = dot(slot_rows, gate_delta, over).astype(BF16)[None]
    up_grad = dot(slot_rows, up_delta, over).astype(BF16)[None]
    down_grad = dot(hidden_low, slot_cot, over).astype(BF16)[None]

    token_grad, weight_grad = pl.pallas_call(
        home_kernel,
        out_shape=(shape((rows, cols)), shape((rows, top), F32)),
        in_specs=[VMEM] * 5,
        out_specs=(VMEM, VMEM),
        cost_estimate=cost(2 * total * rows * cols, 2 * total * cols),
        name="home",
    )(slots, route_weights, home, mix_keep, mix_got)
    return (
        token_grad,
        weight_grad,
        gate_grad,
        up_grad,
        down_grad,
        stacked[:, :mix_hidden],
        stacked[:, mix_hidden : 2 * mix_hidden],
        stacked[:, 2 * mix_hidden :],
    )


def solution(mesh):
    in_specs = (
        P("ep", "tp"),
        P("ep", "tp"),
        P("ep", None),
        P("ep", None),
        P("ep", None, "tp"),
        P("ep", None, "tp"),
        P("ep", "tp", None),
        P(None, "tp"),
        P(None, "tp"),
        P(None, "tp"),
    )
    out_specs = (
        P("ep", "tp"),
        P("ep", None),
        P("ep", None, "tp"),
        P("ep", None, "tp"),
        P("ep", "tp", None),
        P("ep", "tp"),
        P("ep", "tp"),
        P("ep", "tp"),
    )
    return jax.shard_map(
        per_device, mesh=mesh, in_specs=in_specs, out_specs=out_specs, check_vma=False
    )
```

```python
import functools

import jax
import jax.numpy as jnp
from jax import lax
from jax.experimental import pallas as pl
from jax.experimental.pallas import tpu as pltpu
from jax.sharding import PartitionSpec as P


BF16 = jnp.bfloat16
F32 = jnp.float32
LANES = 128
VMEM = pl.BlockSpec(memory_space=pltpu.VMEM)
SMEM = pl.BlockSpec(memory_space=pltpu.SMEM)


def dot(left, right, dims=((1,), (0,))):
    return lax.dot_general(left, right, (dims, ((), ())), preferred_element_type=F32)


class Lazy:
    def __init__(self, ref, copy):
        self.ref, self.copy = ref, copy
        self.pending = False

    def start(self):
        self.copy.start()
        self.pending = True

    def get(self):
        if self.pending:
            self.copy.wait()
            self.pending = False
        return self.ref


def call(body, args, in_kinds, outs, out_kinds, flops, scratch=()):
    n_in, n_out = len(args), len(outs)
    held_in = [i for i in range(n_in) if in_kinds[i] == "h"]
    held_out = [i for i in range(n_out) if out_kinds[i] == "h"]
    held = [(args[i].shape, args[i].dtype) for i in held_in] + [(outs[i].shape, outs[i].dtype) for i in held_out]

    def kernel(*refs):
        ins, results, rest = list(refs[:n_in]), list(refs[n_in : n_in + n_out]), list(refs[n_in + n_out :])
        own, buffers = rest[: len(scratch)], rest[len(scratch) :]
        sems = buffers.pop() if buffers else None
        lazies = []
        for spot, i in enumerate(held_in):
            item = Lazy(buffers[spot], pltpu.make_async_copy(ins[i], buffers[spot], sems.at[spot]))
            item.start()
            ins[i] = item
            lazies.append(item)
        for spot, i in enumerate(held_out, len(held_in)):
            results[i] = Lazy(buffers[spot], pltpu.make_async_copy(buffers[spot], results[i], sems.at[spot]))
            lazies.append(results[i])
        body(*ins, *results, *own)
        for item in lazies:
            item.get()

    in_hbm = pl.BlockSpec(memory_space=pltpu.HBM)
    specs = {"s": SMEM, "v": VMEM, "m": VMEM, "h": in_hbm, "r": in_hbm}
    places = {"m": pltpu.VMEM, "h": pltpu.HBM, "r": pltpu.HBM}
    moved = sum(a.size * a.dtype.itemsize for a in args) + sum(o.size * o.dtype.itemsize for o in outs)
    shapes = list(scratch) + [pltpu.VMEM(dims, dtype) for dims, dtype in held]
    if held:
        shapes.append(pltpu.SemaphoreType.DMA((len(held),)))
    args = [pltpu.with_memory_space_constraint(a, places[k]) if k in places else a for a, k in zip(args, in_kinds)]
    outs = [places[k](o.shape, o.dtype) if k in places else o for o, k in zip(outs, out_kinds)]
    return pl.pallas_call(
        kernel,
        out_shape=tuple(outs),
        in_specs=[specs[k] for k in in_kinds],
        out_specs=tuple(specs[k] for k in out_kinds),
        scratch_shapes=shapes,
        cost_estimate=pl.CostEstimate(flops=flops, bytes_accessed=moved, transcendentals=0),
        compiler_params=pltpu.CompilerParams(vmem_limit_bytes=24 * 1024 * 1024),
    )(*args)


def silu_parts(preact):
    sigmoid_v = jax.nn.sigmoid(preact)
    return (preact * sigmoid_v, sigmoid_v * (1.0 + preact * (1.0 - sigmoid_v)))


def pack_kernel(experts, capacity, routes, weights, *rest):
    sources, packed_out, slots, held, (packed, sems) = rest[:5], rest[5], rest[6], rest[7:12], rest[12:]
    copies = [pltpu.make_async_copy(sources[i], held[i], sems.at[i]) for i in range(5)]
    for copy in copies:
        copy.start()
    tokens, cotangent = held[0], held[1]
    rows, cols = tokens.shape
    total = experts * capacity
    earlier = lax.broadcasted_iota(jnp.int32, (rows, rows), 0) < lax.broadcasted_iota(jnp.int32, (rows, rows), 1)
    name = lax.broadcasted_iota(jnp.int32, (experts, rows), 0)
    routes = routes.get()
    hot0 = (routes[0:1, :] == name).astype(F32)
    hot1 = (routes[1:2, :] == name).astype(F32)
    before = dot((hot0 + hot1).astype(BF16), earlier.astype(F32).astype(BF16))
    slot0 = routes[0:1, :] * capacity + jnp.sum(hot0 * before, axis=0, keepdims=True).astype(jnp.int32)
    slot1 = routes[1:2, :] * capacity + jnp.sum(hot1 * before, axis=0, keepdims=True).astype(jnp.int32)
    slots.ref[0:1, :] = slot0
    slots.ref[1:2, :] = slot1
    slots.start()
    place = lax.broadcasted_iota(jnp.int32, (total, rows), 0)
    pick0 = (place == slot0).astype(F32)
    pick1 = (place == slot1).astype(F32)
    weights = weights.get()
    weight = jnp.sum(pick0 * weights[0:1, :] + pick1 * weights[1:2, :], axis=1, keepdims=True)
    pick = (pick0 + pick1).astype(BF16)
    half = total // 2 // 16 * 16
    parts = ((0, half, 0), (0, half, cols), (half, total, 0), (half, total, cols))
    sent = []
    for spot, (start, stop, left) in enumerate(parts):
        at, lanes = slice(start, stop), slice(left, left + cols)
        if start == 0:
            copies[1 if left else 0].wait()
        value = dot(pick[at], (cotangent if left else tokens)[...])
        packed[at, lanes] = (value * weight[at] if left else value).astype(BF16)
        out = pltpu.make_async_copy(
            packed.at[pl.ds(start, stop - start), pl.ds(left, cols)],
            packed_out.at[pl.ds(start, stop - start), pl.ds(left, cols)],
            sems.at[5 + spot],
        )
        out.start()
        sent.append(out)
    for copy in copies[2:] + sent:
        copy.wait()


def mix_kernel(inner, block, place, own_x, other_x, own_c, other_c, gate, up, down, *factors):
    cols = own_x.shape[1]
    hidden = gate.shape[1]
    core, me = place[0], place[1]
    mine = pl.ds(pl.multiple_of(core * cols, cols), cols)
    theirs = pl.ds(pl.multiple_of((1 - core) * cols, cols), cols)
    pre = dot(own_x[...], gate[mine, :]) + dot(other_x[...], gate[theirs, :])
    mix_up = dot(own_x[...], up[mine, :]) + dot(other_x[...], up[theirs, :])
    back = dot(own_c[...], down[mine, :]) + dot(other_c[...], down[theirs, :])
    act, slope = silu_parts(pre)
    gate_delta = (back * mix_up * slope).astype(BF16)
    up_delta = (back * act).astype(BF16)
    mixed = (act * mix_up).astype(BF16)
    count = cols // block // inner
    width = count * block
    for k in range(inner):
        factor = factors[k] if k else factors[k].ref
        for j in range(count):
            at = pl.ds(pl.multiple_of((j * inner + jnp.bitwise_xor(me % inner, k)) * block, block), block)
            factor[:, j * block : (j + 1) * block] = own_x[:, at]
            factor[:, width + j * block : width + (j + 1) * block] = own_c[:, at]
        factor[:, 2 * width : 2 * width + hidden] = gate_delta
        factor[:, 2 * width + hidden : 2 * width + 2 * hidden] = up_delta
        factor[:, 2 * width + 2 * hidden :] = mixed
        if k == 0:
            factors[k].start()


def mix_back_kernel(core, factor, gate, up, keep, send):
    gate, up, factor = gate.get(), up.get(), factor.get()
    cols = gate.shape[0] // 2
    hidden = gate.shape[1]
    start = factor.shape[1] - 3 * hidden
    mine = pl.ds(pl.multiple_of(core[0] * cols, cols), cols)
    theirs = pl.ds(pl.multiple_of((1 - core[0]) * cols, cols), cols)
    lanes = ((1,), (1,))
    gate_delta, up_delta = factor[:, start : start + hidden], factor[:, start + hidden : start + 2 * hidden]
    send.ref[...] = (dot(gate_delta, gate[theirs, :], lanes) + dot(up_delta, up[theirs, :], lanes)).astype(BF16)
    send.start()
    keep.ref[...] = (dot(gate_delta, gate[mine, :], lanes) + dot(up_delta, up[mine, :], lanes)).astype(BF16)
    keep.start()


def outer_kernel(inner, block, place, *refs):
    factors, other, keep, send, full_x, full_c, grads = refs[:inner], *refs[inner:]
    rows = factors[0].ref.shape[0]
    width = other.shape[1] // 2
    hidden = grads.shape[1] // 3
    core, plane = place[0], place[1] // inner
    mine = pl.ds(pl.multiple_of(core * width, width), width)
    theirs = pl.ds(pl.multiple_of((1 - core) * width, width), width)
    for k in range(inner):
        at = slice(k * rows, (k + 1) * rows)
        full_x[at, theirs] = other[at, :width]
        full_c[at, theirs] = other[at, width:]
    for k in range(inner):
        at = slice(k * rows, (k + 1) * rows)
        factor = factors[k].get()
        full_x[at, mine] = factor[:, :width]
        full_c[at, mine] = factor[:, width : 2 * width]
        grads[at, :] = factor[:, 2 * width :]
    over = ((0,), (0,))
    for parity in (1, 0):
        out = (keep, send)[parity]
        for k in range(parity, 2 * width // block, 2):
            at = pl.ds(pl.multiple_of(jnp.bitwise_xor(plane, k) * block, block), block)
            out.ref[k // 2, :, : 2 * hidden] = dot(full_x[:, at], grads[:, : 2 * hidden], over).astype(out.ref.dtype)
            out.ref[k // 2, :, 2 * hidden :] = dot(full_c[:, at], grads[:, 2 * hidden :], over).astype(out.ref.dtype)
        out.start()


def first_kernel(core, own, gate_in, up_in, down_in, part, gate, up, down, sems):
    cols = own.shape[1] // 2
    hidden = gate.shape[1]
    mine = pl.ds(pl.multiple_of(core[0] * cols, cols), cols)
    theirs = pl.ds(pl.multiple_of((1 - core[0]) * cols, cols), cols)
    copies = []
    for side, at in enumerate((mine, theirs)):
        copies.append(pltpu.make_async_copy(gate_in.at[at, :], gate.at[at, :], sems.at[3 * side]))
        copies.append(pltpu.make_async_copy(up_in.at[at, :], up.at[at, :], sems.at[3 * side + 1]))
        copies.append(pltpu.make_async_copy(down_in.at[:, at], down.at[:, at], sems.at[3 * side + 2]))
    for copy in copies:
        copy.start()
    copies[0].wait()
    part[:, :hidden] = dot(own[:, :cols], gate[mine, :])
    copies[1].wait()
    part[:, hidden : 2 * hidden] = dot(own[:, :cols], up[mine, :])
    copies[2].wait()
    part[:, 2 * hidden :] = dot(own[:, cols:], down[:, mine], ((1,), (1,)))
    for copy in copies[3:]:
        copy.wait()


def second_kernel(core, part, other, gate, up, down, hidden_low, gate_out, up_out, send):
    cols = other.shape[1] // 2
    hidden = gate.shape[1]
    theirs = pl.ds(pl.multiple_of((1 - core[0]) * cols, cols), cols)
    lanes = ((1,), (1,))
    pre = part[:, :hidden] + dot(other[:, :cols], gate[theirs, :])
    up_pre = part[:, hidden : 2 * hidden] + dot(other[:, :cols], up[theirs, :])
    back = part[:, 2 * hidden :] + dot(other[:, cols:], down[:, theirs], lanes)
    act, slope = silu_parts(pre)
    units = act * up_pre
    hidden_low[...] = units.astype(BF16)
    product = jnp.sum(units * back, axis=1, keepdims=True)
    gate_delta = (back * up_pre * slope).astype(BF16)
    up_delta = (back * act).astype(BF16)
    gate_out[...] = gate_delta
    up_out[...] = up_delta
    send[:, :cols] = (dot(gate_delta, gate[theirs, :], lanes) + dot(up_delta, up[theirs, :], lanes)).astype(BF16)
    send[:, cols:] = jnp.broadcast_to(product, (product.shape[0], LANES)).astype(BF16)


def third_kernel(core, hidden_low, gate_delta, up_delta, send, gate, up, keep, hidden_out, gate_out, up_out, sems):
    cols = gate.shape[0] // 2
    mine = pl.ds(pl.multiple_of(core[0] * cols, cols), cols)
    lanes = ((1,), (1,))
    pairs = ((hidden_low, hidden_out), (gate_delta, gate_out), (up_delta, up_out))
    copies = [pltpu.make_async_copy(a, b, sems.at[i]) for i, (a, b) in enumerate(pairs)]
    for copy in copies:
        copy.start()
    keep[:, :cols] = (dot(gate_delta[...], gate[mine, :], lanes) + dot(up_delta[...], up[mine, :], lanes)).astype(BF16)
    keep[:, cols:] = send[:, cols:]
    for copy in copies:
        copy.wait()


def add_kernel(left, right, out):
    out[...] = (left[...].astype(F32) + right[...].astype(F32)).astype(BF16)


def weights_kernel(core, own, other, hidden_low, gate_delta, up_delta, gate_grad, up_grad, down_grad):
    cols = own.ref.shape[1] // 2
    mine = pl.ds(pl.multiple_of(core[0] * cols, cols), cols)
    theirs = pl.ds(pl.multiple_of((1 - core[0]) * cols, cols), cols)
    over = ((0,), (0,))
    own, other, hidden_low, gate_delta, up_delta = (v.get() for v in (own, other, hidden_low, gate_delta, up_delta))
    for side, at in ((own, mine), (other, theirs)):
        gate_grad.ref[at, :] = dot(side[:, :cols], gate_delta[...], over).astype(BF16)
        up_grad.ref[at, :] = dot(side[:, :cols], up_delta[...], over).astype(BF16)
        down_grad.ref[:, at] = dot(hidden_low[...], side[:, cols:], over).astype(BF16)
    gate_grad.start()
    up_grad.start()
    down_grad.start()


def home_kernel(slots, weights, home, mix_a, mix_b, token_grad, weight_grad):
    rows, cols = token_grad.shape
    slots, weights = slots.get(), weights.get()
    place = lax.broadcasted_iota(jnp.int32, (home.shape[0], rows), 0)
    pick0 = (place == slots[0:1, :]).astype(F32)
    pick1 = (place == slots[1:2, :]).astype(F32)
    routed = dot((pick0 + pick1).astype(BF16), home[:, :cols], ((0,), (0,)))
    token_grad[...] = (mix_a.get()[...].astype(F32) + mix_b.get()[...].astype(F32) + routed).astype(BF16)
    tail = home[:, cols:].astype(F32)[:, 0:1]
    weight_grad[0:1, :] = jnp.sum(pick0 * tail, axis=0, keepdims=True) / weights[0:1, :]
    weight_grad[1:2, :] = jnp.sum(pick1 * tail, axis=0, keepdims=True) / weights[1:2, :]


def shape(dims, dtype=BF16):
    return jax.ShapeDtypeStruct(dims, dtype)


def ordered(core, own, other):
    return jnp.concatenate([jnp.where(core == 0, own, other), jnp.where(core == 0, other, own)], axis=1)


def per_device(
    tokens,
    cotangent,
    routes,
    route_weights,
    gate_proj,
    up_proj,
    down_proj,
    shared_gate,
    shared_up,
    shared_down,
):
    groups = lax.axis_size("ep")
    halves = lax.axis_size("tp")
    assert halves == 2 and gate_proj.shape[0] == 1
    me, core = lax.axis_index("ep"), lax.axis_index("tp")
    experts = groups
    rows, top = routes.shape
    assert top == 2
    cols = tokens.shape[1]
    hidden = gate_proj.shape[2]
    mix_hidden = shared_gate.shape[1]
    assigned = rows * top
    capacity = assigned // experts + assigned // (2 * experts)
    total = experts * capacity
    core_arr = core.astype(jnp.int32).reshape(1)
    place_arr = jnp.stack([core, me]).astype(jnp.int32)
    inner = 4
    block = 2 * cols // groups
    bits = groups.bit_length() - 1
    paired = groups == 1 << bits and groups > inner and block % LANES == 0 and cols % (inner * block) == 0

    def swap(value):
        return lax.ppermute(value, "tp", [(0, 1), (1, 0)])

    def cross(value, step):
        return lax.ppermute(value, "ep", [(i, i ^ step) for i in range(groups)])

    flops = 2 * total * cols * hidden
    mix_flops = 2 * rows * cols * mix_hidden
    other_x, other_c = swap(tokens), swap(cotangent)
    packed, slots, *held = call(
        functools.partial(pack_kernel, experts, capacity),
        (routes.T, route_weights.T, tokens, cotangent, shared_gate, shared_up, shared_down),
        "hhrrrrr",
        (shape((total, 2 * cols)), shape((top, rows), jnp.int32))
        + (shape(tokens.shape),) * 2
        + (shape(shared_gate.shape),) * 3,
        "rhmmmmm",
        4 * total * rows * cols,
        [pltpu.VMEM((total, 2 * cols), BF16), pltpu.SemaphoreType.DMA((9,))],
    )
    got = lax.all_to_all(
        packed.reshape(groups, capacity, 2 * cols), "ep", split_axis=0, concat_axis=0, tiled=True
    ).reshape(total, 2 * cols)

    split, spot = (inner, block) if paired else (1, cols)
    width = cols // split
    factors = list(
        call(
            functools.partial(mix_kernel, split, spot),
            (place_arr, held[0], other_x, held[1], other_c, *held[2:]),
            "smvmvmmm",
            (shape((rows, 2 * width + 3 * mix_hidden)),) * split,
            "h" + "m" * (split - 1),
            6 * mix_flops,
        )
    )
    mix_keep, mix_send = call(
        mix_back_kernel,
        (core_arr, factors[0], shared_gate, shared_up),
        "shhh",
        (shape((rows, cols)),) * 2,
        "hh",
        4 * mix_flops,
    )
    mix_got = swap(mix_send)
    if paired:
        for k in range(1, inner):
            factors[k] = cross(factors[k], k)
        other = swap(jnp.concatenate([value[:, : 2 * width] for value in factors], axis=0))
        planes = groups // inner
        keep, send = call(
            functools.partial(outer_kernel, inner, block),
            (place_arr, *factors, other),
            "s" + "h" * inner + "v",
            (shape((planes // 2, block, 3 * mix_hidden), F32), shape((planes // 2, block, 3 * mix_hidden))),
            "hh",
            6 * mix_flops,
            [pltpu.VMEM((inner * rows, 2 * width), BF16)] * 2 + [pltpu.VMEM((inner * rows, 3 * mix_hidden), BF16)],
        )
        step = inner
        while step < groups:
            value = keep + cross(send, step).astype(F32)
            step *= 2
            if step < groups:
                pairs = value.reshape((-1, 2) + value.shape[1:])
                keep, send = pairs[:, 0], pairs[:, 1].astype(BF16)
        stacked = value[0]
    else:
        whole_x, whole_c = ordered(core, tokens, other_x), ordered(core, cotangent, other_c)
        grads = factors[0][:, 2 * width :]
        stacked = lax.psum_scatter(
            jnp.concatenate(
                [dot(whole_x, grads[:, : 2 * mix_hidden], ((0,), (0,))), dot(whole_c, grads[:, 2 * mix_hidden :], ((0,), (0,)))],
                axis=1,
            ),
            "ep",
            scatter_dimension=0,
            tiled=True,
        )

    gate, up, down = gate_proj[0], up_proj[0], down_proj[0]
    got_other = swap(got)
    part, *held = call(
        first_kernel,
        (core_arr, got, gate, up, down),
        "svrrr",
        (shape((total, 3 * hidden), F32), shape(gate.shape), shape(up.shape), shape(down.shape)),
        "mmmm",
        3 * flops,
        [pltpu.SemaphoreType.DMA((6,))],
    )
    deltas = (shape((total, hidden)),) * 3
    *low, send = call(
        second_kernel,
        (core_arr, part, got_other, *held),
        "smvmmm",
        deltas + (shape((total, cols + LANES)),),
        "mmmm",
        5 * flops,
    )
    received = swap(send)
    keep, hidden_low, gate_delta, up_delta = call(
        third_kernel,
        (core_arr, *low, send, held[0], held[1]),
        "smmmmmm",
        (shape((total, cols + LANES)),) + deltas,
        "mrrr",
        2 * flops,
        [pltpu.SemaphoreType.DMA((3,))],
    )
    (back,) = call(add_kernel, (keep, received), "mv", (shape((total, cols + LANES)),), "v", total * cols)
    home = lax.all_to_all(
        back.reshape(groups, capacity, cols + LANES), "ep", split_axis=0, concat_axis=0, tiled=True
    ).reshape(total, cols + LANES)
    gate_grad, up_grad, down_grad = call(
        weights_kernel,
        (core_arr, got, got_other, hidden_low, gate_delta, up_delta),
        "shhhhh",
        (shape((2 * cols, hidden)),) * 2 + (shape((hidden, 2 * cols)),),
        "hhh",
        6 * flops,
    )
    token_grad, weight_grad = call(
        home_kernel,
        (slots, route_weights.T, home, mix_keep, mix_got),
        "hhvhh",
        (shape((rows, cols)), shape((top, rows), F32)),
        "vv",
        2 * total * rows * cols,
    )
    return (
        token_grad,
        weight_grad.T,
        gate_grad[None],
        up_grad[None],
        down_grad[None],
        stacked[:, :mix_hidden],
        stacked[:, mix_hidden : 2 * mix_hidden],
        stacked[:, 2 * mix_hidden :],
    )


def solution(mesh):
    in_specs = (
        P("ep", "tp"),
        P("ep", "tp"),
        P("ep", None),
        P("ep", None),
        P("ep", None, "tp"),
        P("ep", None, "tp"),
        P("ep", "tp", None),
        P(None, "tp"),
        P(None, "tp"),
        P(None, "tp"),
    )
    out_specs = (
        P("ep", "tp"),
        P("ep", None),
        P("ep", None, "tp"),
        P("ep", None, "tp"),
        P("ep", "tp", None),
        P("ep", "tp"),
        P("ep", "tp"),
        P("ep", "tp"),
    )

    return jax.shard_map(per_device, mesh=mesh, in_specs=in_specs, out_specs=out_specs, check_vma=False)
```
